32 devices in a mesh: ep: 8 (over z, core), tp: 4 (over y, x).
Axes of the slice: x: 2, y: 2, z: 4, core: 2. Of those that a mesh axis runs over, the one named last changes fastest.
Arguments:
- tokens: bfloat16 [512, 2048], P('ep'), may hold values from -6 to 6
- mix_gain: float32 [2048], replicated, may hold values from 0.1 to 1.9
- w_in: bfloat16 [2048, 1024], P(None, 'tp'), may hold values from -0.125 to 0.125
- decay_re: float32 [64, 64], P('tp'), may hold values from -1 to -0.1
- freq: float32 [64, 64], P('tp'), may hold values from 0 to 100
- log_step: float32 [64], P('tp'), may hold values from -3.9 to 0
- in_re: bfloat16 [64, 16, 64], P('tp'), may hold values from -1 to 1
- in_im: bfloat16 [64, 16, 64], P('tp'), may hold values from -1 to 1
- out_re: bfloat16 [64, 16, 64], P('tp'), may hold values from -0.75 to 0.75
- out_im: bfloat16 [64, 16, 64], P('tp'), may hold values from -0.75 to 0.75
- skip: float32 [64, 16], P('tp'), may hold values from -4 to 4
- state_re: float32 [512, 64, 64], P('ep', 'tp'), may hold values from -6 to 6
- state_im: float32 [512, 64, 64], P('ep', 'tp'), may hold values from -6 to 6
- glu_weight: bfloat16 [1024, 1024], P(None, 'tp'), may hold values from -0.1875 to 0.1875
- glu_bias: float32 [1024], P('tp'), may hold values from -4 to 4
- out_weight: bfloat16 [1024, 2048], P('tp'), may hold values from -0.1875 to 0.1875
- ffn_gain: float32 [2048], replicated, may hold values from 0.1 to 1.9
- route: int32 [512, 2], P('ep'), may hold values from 0 to 7, all different within a row; in each aligned block of 64 rows (0 to 63, 64 to 127, ...) at most 24 rows name the same one
- route_weight: float32 [512, 2], P('ep'), may hold values from 0.2 to 1
- expert_gate: bfloat16 [8, 2048, 3584], P('ep', None, 'tp'), may hold values from -0.125 to 0.125
- expert_up: bfloat16 [8, 2048, 3584], P('ep', None, 'tp'), may hold values from -0.125 to 0.125
- expert_down: bfloat16 [8, 3584, 2048], P('ep', 'tp'), may hold values from -0.09375 to 0.09375
Outputs:
- mixed: bfloat16 [512, 2048], P('ep', 'tp')
- new_re: float32 [512, 64, 64], P('ep', 'tp')
- new_im: float32 [512, 64, 64], P('ep', 'tp')
The draws below stay inside these ranges and needn't reach their ends.
Inputs may be any that keep to these rules, and one draw needn't show every extreme that they name: `route`: each row names 2 different experts. Within the 64 rows of one index of ep no expert is named more than 24 times, and in every draw some expert is named exactly 24 times by the rows of some index of ep.
All inputs are finite; a program needn't handle non-finite values.
Results may differ from the reference program's by a relative error of at most 0.015.
Values may be sent and summed in bfloat16 or wider, within the bound.
A program may use at most 64 MiB of HBM per device.

```python
import math
import jax
import jax.numpy as jnp
import numpy as np
from jax import lax

D = 2048
C = 1024
H = 16
P_SIZE = 64
FFE = 3584
TOPK = 2
SEQ_GRP = 64
G = 64
EXPERTS = 8
SEQS = 512
CAP = 24
ROWS_E = 192
N_TP = 4


def levels(rng, shape, pieces, low, largest):
    def one(dim, blocks):
        heights = jax.random.uniform(jax.random.fold_in(jax.random.fold_in(rng, 6), dim), (blocks,), jnp.float32, low / len(pieces), largest / len(pieces))
        return jnp.repeat(jnp.exp(heights), shape[dim] // blocks).reshape((-1,) + (1,) * (len(shape) - dim - 1))

    level = one(*pieces[0])
    for cut in pieces[1:]:
        level = level * one(*cut)
    return level


def routed_block(key, own, number, rows, count, top, bound, lean):
    ranking = jax.random.permutation(key, count)
    crowded, usual = portions_of(count, rows * top, bound, lean, True), portions_of(count, rows * top, bound, lean, False)
    places = jnp.arange(count)

    def named(tallies, turn):
        used = int((tallies > 0).sum())
        fixed = max(1, used // 4)
        moved = fixed + (places - fixed + turn * (used - fixed)) % max(1, count - fixed)
        return jnp.zeros((count,), jnp.int32).at[ranking[jnp.where(places < fixed, places, moved)]].set(jnp.asarray(tallies, jnp.int32))

    tallies = jnp.where(number % 4 == 0, named(crowded, number // 4), named(usual, number - number // 4 - 1))
    mixed = jax.random.permutation(jax.random.fold_in(own, 3), count)
    donor, taker = mixed[0:count // 2 * 2:2], mixed[1:count // 2 * 2:2]
    margin = jnp.minimum(tallies[donor] - 1, bound - tallies[taker]) // 2
    margin = jnp.where((donor == ranking[0]) | (taker == ranking[0]) | (tallies[taker] == 0), 0, jnp.maximum(margin, 0))
    moved = jax.random.randint(jax.random.fold_in(own, 4), (count // 2,), 0, 1 << 20) % (margin + 1)
    tallies = tallies.at[donor].add(-moved).at[taker].add(moved)
    members = jnp.searchsorted(jnp.cumsum(tallies), jnp.arange(rows * top), side="right").astype(jnp.int32)
    listing = members.reshape(top, rows).T
    listing = listing[jax.random.permutation(jax.random.fold_in(own, 1), rows)]
    turn = jax.random.randint(jax.random.fold_in(own, 2), (rows, 1), 0, top)
    return jnp.take_along_axis(listing, (jnp.arange(top)[None, :] + turn) % top, axis=1)


def portions_of(amount, total, bound, slope, full):
    loads = [(1 << 20) // math.isqrt(rank ** slope) + 1 for rank in range(1, amount + 1)]
    largest = bound if full else min(bound, max(-(-total // amount), total * loads[0] // sum(loads)))
    least = 1 if total - largest >= amount - 1 else 0
    holding, spare = [largest] + [least] * (amount - 1), total - largest - least * (amount - 1)
    while spare > 0:
        candidates = [i for i in range(1, amount) if holding[i] < largest] or [i for i in range(1, amount) if holding[i] < bound]
        whole, budget = sum([loads[i] for i in candidates]), spare
        for i in candidates:
            addition = min(bound - holding[i], max(1, budget * loads[i] // whole), spare)
            holding[i] = holding[i] + addition
            spare = spare - addition
    return np.array(holding)


def bell_draw(rng, shape, spread, most, split=(), kind=jnp.bfloat16):
    level = levels(rng, shape, split, -0.22, 0.18) if split else 1.0
    entries = jax.random.normal(rng, shape, jnp.float32) * spread * level
    return jnp.minimum(jnp.maximum(entries, -most), most).astype(kind)


def setup_inputs(seed: int = 0) -> dict:
    splits = jax.random.split(jax.random.key(seed), 23)
    tokens = bell_draw(splits[0], (SEQS, D), 1.0, 6.0, ((0, 8),))
    mix_gain = jnp.clip(1.0 + 0.18 * jax.random.normal(splits[1], (D,), jnp.float32), 0.1, 1.9)
    w_in = bell_draw(splits[2], (D, C), D ** -0.5, 0.125, ((1, 4),))
    decay_re = jnp.clip(-1.0 + 0.9 * jax.random.uniform(splits[3], (G, P_SIZE), jnp.float32) ** levels(splits[3], (G, P_SIZE), ((0, 4),), -0.2, 0.2), -1.0, -0.1)
    freq = jnp.clip(100.0 * jax.random.uniform(splits[4], (G, P_SIZE), jnp.float32) ** levels(splits[4], (G, P_SIZE), ((0, 4),), -0.2, 0.2), 0.0, 100.0)
    log_step = jnp.clip(-3.9 + 3.9 * jax.random.uniform(splits[5], (G,), jnp.float32) ** levels(splits[5], (G,), ((0, 4),), -0.2, 0.2), -3.9, 0.0)
    in_re = bell_draw(splits[6], (G, H, P_SIZE), (2 * H) ** -0.5, 1.0, ((0, 4),))
    in_im = bell_draw(splits[7], (G, H, P_SIZE), (2 * H) ** -0.5, 1.0, ((0, 4),))
    out_re = bell_draw(splits[8], (G, H, P_SIZE), P_SIZE ** -0.5, 0.75, ((0, 4),))
    out_im = bell_draw(splits[9], (G, H, P_SIZE), P_SIZE ** -0.5, 0.75, ((0, 4),))
    skip = bell_draw(splits[10], (G, H), 1.0, 4.0, ((0, 4),), jnp.float32)
    state_re = bell_draw(splits[11], (SEQS, G, P_SIZE), 1.0, 6.0, ((0, 8), (1, 4)), jnp.float32)
    state_im = bell_draw(splits[12], (SEQS, G, P_SIZE), 1.0, 6.0, ((0, 8), (1, 4)), jnp.float32)
    glu_weight = bell_draw(splits[13], (C, C), C ** -0.5, 0.1875, ((1, 4),))
    glu_bias = bell_draw(splits[14], (C,), 1.0, 4.0, ((0, 4),), jnp.float32)
    out_weight = bell_draw(splits[15], (C, D), C ** -0.5, 0.1875, ((0, 4),))
    ffn_gain = jnp.clip(1.0 + 0.18 * jax.random.normal(splits[16], (D,), jnp.float32), 0.1, 1.9)
    route_keys = jax.random.split(jax.random.fold_in(splits[17], 1), SEQS // SEQ_GRP)
    route_turns = jax.random.permutation(jax.random.fold_in(splits[17], 3), SEQS // SEQ_GRP)
    route = jax.vmap(lambda own, number: routed_block(jax.random.fold_in(splits[17], 2), own, number, SEQ_GRP, EXPERTS, TOPK, CAP, 2))(route_keys, route_turns).reshape((SEQS, TOPK))
    route_weight = jnp.clip(0.2 + 0.8 * jax.random.uniform(splits[18], (SEQS, TOPK), jnp.float32) ** levels(splits[18], (SEQS, TOPK), ((0, 8),), -0.2, 0.2), 0.2, 1.0)
    expert_gate = bell_draw(splits[19], (EXPERTS, D, FFE), D ** -0.5, 0.125, ((0, 8), (2, 4)))
    expert_up = bell_draw(splits[20], (EXPERTS, D, FFE), D ** -0.5, 0.125, ((0, 8), (2, 4)))
    expert_down = bell_draw(splits[21], (EXPERTS, FFE, D), FFE ** -0.5, 0.09375, ((0, 8), (1, 4)))
    return {"tokens": tokens, "mix_gain": mix_gain, "w_in": w_in, "decay_re": decay_re, "freq": freq, "log_step": log_step, "in_re": in_re, "in_im": in_im, "out_re": out_re, "out_im": out_im, "skip": skip, "state_re": state_re, "state_im": state_im, "glu_weight": glu_weight, "glu_bias": glu_bias, "out_weight": out_weight, "ffn_gain": ffn_gain, "route": route, "route_weight": route_weight, "expert_gate": expert_gate, "expert_up": expert_up, "expert_down": expert_down}


norm_eps = 1e-06

def rms_scale(rows, gain):
    values = rows.astype(jnp.float32)
    scaled = values * lax.rsqrt(lax.optimization_barrier(jnp.mean(values * values, axis=-1, keepdims=True)) + norm_eps)
    return (scaled * gain).astype(jnp.bfloat16)

def split_sum(left, right, parts):
    width = left.shape[1] // parts
    lefts = jnp.moveaxis(left.reshape(left.shape[0], parts, width), 1, 0)
    rights = right.reshape(parts, width, right.shape[1])

    def add_block(total, pair):
        term = jnp.dot(pair[0], pair[1], preferred_element_type=jnp.float32).astype(jnp.bfloat16)
        term = lax.optimization_barrier(term)
        return (total + term.astype(jnp.float32), None)
    start = jnp.zeros((left.shape[0], right.shape[1]), jnp.float32)
    total, _ = lax.scan(add_block, start, (lefts, rights))
    return total

def state_step(inputs, state_re, state_im, decay_re, freq, log_step, in_re, in_im, out_re, out_im, skip):
    highest = lax.Precision.HIGHEST
    step = jnp.exp(log_step)[:, None]
    magnitude = jnp.exp(decay_re * step)
    turn_re = magnitude * jnp.cos(freq * step)
    turn_im = magnitude * jnp.sin(freq * step)
    denom = decay_re * decay_re + freq * freq
    coef_re = ((turn_re - 1.0) * decay_re + turn_im * freq) / denom
    coef_im = (turn_im * decay_re - (turn_re - 1.0) * freq) / denom
    values = inputs.astype(jnp.float32)
    drive_re = jnp.einsum('sgh,ghp->sgp', values, in_re.astype(jnp.float32), precision=highest)
    drive_im = jnp.einsum('sgh,ghp->sgp', values, in_im.astype(jnp.float32), precision=highest)
    push_re = coef_re * drive_re - coef_im * drive_im
    push_im = coef_re * drive_im + coef_im * drive_re
    new_re = turn_re * state_re - turn_im * state_im + push_re
    new_im = turn_re * state_im + turn_im * state_re + push_im
    read = jnp.einsum('ghp,sgp->sgh', out_re.astype(jnp.float32), new_re, precision=highest)
    read = read - jnp.einsum('ghp,sgp->sgh', out_im.astype(jnp.float32), new_im, precision=highest)
    read = read + skip * values
    return (read, new_re, new_im)

def reference(tokens, mix_gain, w_in, decay_re, freq, log_step, in_re, in_im, out_re, out_im, skip, state_re, state_im, glu_weight, glu_bias, out_weight, ffn_gain, route, route_weight, expert_gate, expert_up, expert_down):
    normed = rms_scale(tokens, mix_gain)
    drive = jnp.dot(normed, w_in, preferred_element_type=jnp.float32).astype(jnp.bfloat16)
    inputs = drive.reshape(SEQS, G, H)
    read, new_re, new_im = state_step(inputs, state_re, state_im, decay_re, freq, log_step, in_re, in_im, out_re, out_im, skip)
    mixed_in = jax.nn.gelu(read).reshape(SEQS, C).astype(jnp.bfloat16)
    gate = jnp.dot(mixed_in, glu_weight, preferred_element_type=jnp.float32) + glu_bias
    gated = (mixed_in.astype(jnp.float32) * jax.nn.sigmoid(gate)).astype(jnp.bfloat16)
    mix_total = split_sum(gated, out_weight, N_TP)
    resid = (tokens.astype(jnp.float32) + mix_total).astype(jnp.bfloat16)
    normed2 = rms_scale(resid, ffn_gain)
    flat_route = route.reshape(-1)
    flat_weight = route_weight.reshape(-1)

    def expert_pass(total, inputs_e):
        gate_w, up_w, down_w, index = inputs_e
        hits = flat_route == index
        picked = jnp.nonzero(hits, size=ROWS_E, fill_value=0)[0].astype(jnp.int32)
        valid = (jnp.arange(ROWS_E) < jnp.sum(hits.astype(jnp.int32))).astype(jnp.float32)
        token_ids = (picked // TOPK).astype(jnp.int32)
        rows = normed2[token_ids]
        gate_e = jnp.dot(rows, gate_w, preferred_element_type=jnp.float32)
        up_e = jnp.dot(rows, up_w, preferred_element_type=jnp.float32)
        hidden = (jax.nn.silu(gate_e) * up_e).astype(jnp.bfloat16)
        result = split_sum(hidden, down_w, N_TP).astype(jnp.bfloat16)
        weight = flat_weight[picked] * valid
        total = total.at[token_ids].add(weight[:, None] * result.astype(jnp.float32))
        return (total, None)
    start = resid.astype(jnp.float32)
    indices = jnp.arange(EXPERTS).astype(jnp.int32)
    total, _ = lax.scan(expert_pass, start, (expert_gate, expert_up, expert_down, indices))
    return (total.astype(jnp.bfloat16), new_re, new_im)
```

```python
import functools
import jax
import jax.numpy as jnp
from jax import lax
from jax.experimental import pallas as pl
from jax.experimental.pallas import tpu as pltpu
from jax.sharding import PartitionSpec as P

norm_eps = 1e-06
MESH = pl.DeviceIdType.MESH


def rms_scale(rows, gain):
    values = rows.astype(jnp.float32)
    scaled = values * lax.rsqrt(jnp.mean(values * values, axis=-1, keepdims=True) + norm_eps)
    return (scaled * gain).astype(jnp.bfloat16)


def state_step(
    inputs, state_re, state_im, decay_re, freq, log_step, in_re, in_im, out_re, out_im, skip
):
    highest = lax.Precision.HIGHEST
    step = jnp.exp(log_step)[:, None]
    magnitude = jnp.exp(decay_re * step)
    turn_re = magnitude * jnp.cos(freq * step)
    turn_im = magnitude * jnp.sin(freq * step)
    denom = decay_re * decay_re + freq * freq
    coef_re = ((turn_re - 1.0) * decay_re + turn_im * freq) / denom
    coef_im = (turn_im * decay_re - (turn_re - 1.0) * freq) / denom
    drive_re = jnp.einsum("sgh,ghp->sgp", inputs, in_re, preferred_element_type=jnp.float32)
    drive_im = jnp.einsum("sgh,ghp->sgp", inputs, in_im, preferred_element_type=jnp.float32)
    push_re = coef_re * drive_re - coef_im * drive_im
    push_im = coef_re * drive_im + coef_im * drive_re
    new_re = turn_re * state_re - turn_im * state_im + push_re
    new_im = turn_re * state_im + turn_im * state_re + push_im
    read = jnp.einsum("ghp,sgp->sgh", out_re.astype(jnp.float32), new_re, precision=highest)
    read = read - jnp.einsum("ghp,sgp->sgh", out_im.astype(jnp.float32), new_im, precision=highest)
    read = read + skip * inputs.astype(jnp.float32)
    return (read, new_re, new_im)


def remote(src, dst, send, recv, axis, peer):
    copy = pltpu.make_async_remote_copy(
        src_ref=src,
        dst_ref=dst,
        send_sem=send,
        recv_sem=recv,
        device_id={axis: peer},
        device_id_type=MESH,
    )
    copy.start()


def drain(ref, sem):
    pltpu.make_async_copy(ref, ref, sem).wait()


def near_first(index, count):
    half = (index + 1) // 2
    odd = index % 2
    return half * odd + (count - half) * (1 - odd)


def exchange(
    n_tp,
    n_ep,
    mixed_ref,
    tokens_ref,
    glu_ref,
    bias_ref,
    out_w_ref,
    gain_ref,
    select_ref,
    combine_ref,
    gate_hbm,
    up_hbm,
    down_hbm,
    out_ref,
    gate_w,
    up_w,
    down_w,
    ag_buf,
    rs_out,
    rs_in,
    disp,
    rows,
    xn,
    back_out,
    back_own,
    back_in,
    ret_out,
    ret_in,
    w_sem,
    ag_s,
    ag_r,
    rs_s,
    rs_r,
    disp_s,
    disp_r,
    fwd_s,
    fwd_r,
    back_s,
    back_r,
    ret_s,
    ret_r,
):
    tp = lax.axis_index("tp")
    ep = lax.axis_index("ep")
    seqs, chan = mixed_ref.shape
    width = out_ref.shape[1]
    groups = rows.shape[2]
    slots = n_ep * groups * 8
    hidden_n = gate_w.shape[1]
    f32 = jnp.float32
    bf16 = jnp.bfloat16

    loads = [
        pltpu.make_async_copy(src.at[0], dst, w_sem.at[i])
        for i, (src, dst) in enumerate(((gate_hbm, gate_w), (up_hbm, up_w), (down_hbm, down_w)))
    ]
    for load in loads:
        load.start()

    barrier = pltpu.get_barrier_semaphore()

    @pl.loop(1, n_tp)
    def _(k):
        pl.semaphore_signal(
            barrier, inc=1, device_id={"tp": lax.rem(tp + k, n_tp)}, device_id_type=MESH
        )

    @pl.loop(1, n_ep)
    def _(k):
        pl.semaphore_signal(
            barrier, inc=1, device_id={"ep": lax.rem(ep + k, n_ep)}, device_id_type=MESH
        )

    pl.semaphore_wait(barrier, n_tp + n_ep - 2)

    def peer_at(k):
        return lax.rem(tp + k, n_tp)

    def source_at(k):
        return lax.rem(tp + n_tp - k, n_tp)

    for k in range(1, n_tp):
        remote(mixed_ref, ag_buf.at[k - 1], ag_s.at[k - 1], ag_r.at[k - 1], "tp", peer_at(k))

    def glu_rows(owner):
        return glu_ref[pl.ds(pl.multiple_of(owner * chan, chan), chan), :]

    mixed = mixed_ref[...]
    gate = jnp.dot(mixed, glu_rows(tp), preferred_element_type=f32) + bias_ref[...]
    for k in range(1, n_tp):
        drain(ag_buf.at[k - 1], ag_r.at[k - 1])
        gate += jnp.dot(ag_buf[k - 1], glu_rows(source_at(k)), preferred_element_type=f32)
    gated = (mixed.astype(f32) * jax.nn.sigmoid(gate)).astype(bf16)

    def columns(owner):
        return pl.ds(pl.multiple_of(owner * width, width), width)

    for k in range(1, n_tp):
        part = jnp.dot(gated, out_w_ref[:, columns(peer_at(k))], preferred_element_type=f32)
        rs_out[k - 1] = part.astype(bf16)
        remote(
            rs_out.at[k - 1], rs_in.at[k - 1], rs_s.at[k - 1], rs_r.at[k - 1], "tp", peer_at(k)
        )
    total = jnp.dot(gated, out_w_ref[:, columns(tp)], preferred_element_type=f32)
    total = total.astype(bf16).astype(f32)
    for k in range(1, n_tp):
        drain(rs_in.at[k - 1], rs_r.at[k - 1])
        total += rs_in[k - 1].astype(f32)
    resid = (tokens_ref[:, columns(tp)].astype(f32) + total).astype(bf16)

    picked = jnp.dot(select_ref[...], resid, preferred_element_type=f32)
    disp[...] = picked.reshape(n_ep, groups, 8, width).astype(bf16)

    @pl.loop(1, n_ep)
    def _(i):
        to = lax.rem(ep + near_first(i, n_ep), n_ep)
        remote(disp.at[to], rows.at[tp, ep], disp_s, disp_r.at[i - 1], "ep", to)

    rows[tp, ep] = disp[ep]

    def forward(block):
        for k in range(1, n_tp):
            here = rows.at[tp, block]
            remote(here, here, fwd_s.at[k - 1], fwd_r.at[k - 1], "tp", peer_at(k))

    for k in range(1, n_tp):
        remote(
            disp.at[ep], rows.at[tp, ep], fwd_s.at[k - 1], fwd_r.at[k - 1], "tp", peer_at(k)
        )

    @pl.loop(1, n_ep)
    def _(i):
        block = lax.rem(ep + n_ep - near_first(i, n_ep), n_ep)
        drain(rows.at[tp, block], disp_r.at[i - 1])
        forward(block)

    def row_values(owner):
        return rows[owner].astype(f32).reshape(slots, width)

    values = row_values(tp)
    squares = jnp.sum(values * values, axis=1, keepdims=True)
    for k in range(1, n_tp):
        drain(rows.at[source_at(k)], fwd_r.at[k - 1])
        values = row_values(source_at(k))
        squares += jnp.sum(values * values, axis=1, keepdims=True)
    scale = lax.rsqrt(squares / (n_tp * width) + norm_eps)
    for owner in range(n_tp):
        cols = pl.ds(owner * width, width)
        xn[:, cols] = (row_values(owner) * scale * gain_ref[:, cols]).astype(bf16)

    loads[0].wait()
    loads[1].wait()
    pieces = []
    for start in range(0, hidden_n, 256):
        cols = pl.ds(start, min(256, hidden_n - start))
        gate_h = jnp.dot(xn[...], gate_w[:, cols], preferred_element_type=f32)
        up_h = jnp.dot(xn[...], up_w[:, cols], preferred_element_type=f32)
        pieces.append((jax.nn.silu(gate_h) * up_h).astype(bf16))
    hidden = jnp.concatenate(pieces, axis=1)
    loads[2].wait()

    def down(owner):
        part = jnp.dot(hidden, down_w[:, columns(owner)], preferred_element_type=f32)
        return part.reshape(n_ep, groups, 8, width).astype(bf16)

    for k in range(1, n_tp):
        back_out[k - 1] = down(peer_at(k))

        @pl.loop(1, n_ep + 1)
        def _(i):
            block = lax.rem(ep + near_first(i, n_ep) * (i // n_ep * -1 + 1), n_ep)
            remote(
                back_out.at[k - 1, block],
                back_in.at[block, k - 1],
                back_s.at[k - 1],
                back_r.at[block],
                "tp",
                peer_at(k),
            )

    back_own[...] = down(tp)

    def settled(block):
        drain(back_in.at[block], back_r.at[block])
        result = back_own[block].astype(f32)
        for k in range(1, n_tp):
            result += back_in[block, k - 1].astype(f32)
        return result.astype(bf16)

    @pl.loop(1, n_ep)
    def _(i):
        to = lax.rem(ep + near_first(i, n_ep), n_ep)
        ret_out[to] = settled(to)
        remote(ret_out.at[to], ret_in.at[ep], ret_s, ret_r.at[i - 1], "ep", to)

    ret_in[ep] = settled(ep)

    @pl.loop(1, n_ep)
    def _(i):
        block = lax.rem(ep + n_ep - near_first(i, n_ep), n_ep)
        drain(ret_in.at[block], ret_r.at[i - 1])

    returned = ret_in[...].astype(f32).reshape(slots, width)
    expert_total = jnp.dot(
        combine_ref[...], returned, precision=lax.Precision.HIGHEST, preferred_element_type=f32
    )
    out_ref[...] = (resid.astype(f32) + expert_total).astype(bf16)

    for k in range(1, n_tp):
        drain(mixed_ref, ag_s.at[k - 1])
        drain(rs_out.at[k - 1], rs_s.at[k - 1])
        drain(rows.at[0], fwd_s.at[k - 1])
        drain(back_out.at[k - 1], back_s.at[k - 1])
    drain(disp.at[pl.ds(0, n_ep - 1)], disp_s)
    drain(ret_out.at[pl.ds(0, n_ep - 1)], ret_s)


def local(
    tokens,
    mix_gain,
    w_in,
    decay_re,
    freq,
    log_step,
    in_re,
    in_im,
    out_re,
    out_im,
    skip,
    state_re,
    state_im,
    glu_weight,
    glu_bias,
    out_weight,
    ffn_gain,
    route,
    route_weight,
    expert_gate,
    expert_up,
    expert_down,
):
    seq_count, model_width = tokens.shape
    groups_local = decay_re.shape[0]
    n_tp = lax.axis_size("tp")
    experts = lax.axis_size("ep")
    local_width = model_width // n_tp
    top_count = route.shape[1]
    hidden_n = expert_gate.shape[2]
    slot_cap = (3 * seq_count * top_count + 2 * experts - 1) // (2 * experts)
    slot_rows = (slot_cap + 7) // 8 * 8
    slots = experts * slot_rows
    normed = rms_scale(tokens, mix_gain)
    drive = jnp.dot(normed, w_in, preferred_element_type=jnp.float32).astype(jnp.bfloat16)
    inputs = drive.reshape(seq_count, groups_local, -1)
    read, new_re, new_im = state_step(
        inputs, state_re, state_im, decay_re, freq, log_step, in_re, in_im, out_re, out_im, skip
    )
    mixed_in = jax.nn.gelu(read).reshape(seq_count, -1).astype(jnp.bfloat16)
    hits = (route[:, :, None] == jnp.arange(experts)[None, None, :]).astype(jnp.float32)
    earlier = jnp.tril(jnp.ones((seq_count, seq_count), jnp.float32), -1)
    before = jnp.dot(earlier, jnp.sum(hits, axis=1))
    rank = jnp.sum(before[:, None, :] * hits, axis=2).astype(jnp.int32)
    slot = route * slot_rows + rank
    picks = slot[:, :, None] == jnp.arange(slots)[None, None, :]
    combine = jnp.sum(jnp.where(picks, route_weight[:, :, None], 0.0), axis=1)
    select = jnp.any(slot.T[None, :, :] == jnp.arange(slots)[:, None, None], axis=1)
    chan = mixed_in.shape[1]
    block = (slot_rows // 8, 8, local_width)
    bf16 = jnp.bfloat16
    dma = pltpu.SemaphoreType.DMA
    vmem = pl.BlockSpec(memory_space=pltpu.VMEM)
    anyplace = pl.BlockSpec(memory_space=pl.ANY)
    mixed = pl.pallas_call(
        functools.partial(exchange, n_tp, experts),
        out_shape=jax.ShapeDtypeStruct((seq_count, local_width), bf16),
        in_specs=[vmem] * 8 + [anyplace] * 3,
        out_specs=vmem,
        scratch_shapes=[
            pltpu.VMEM((model_width, hidden_n), bf16),
            pltpu.VMEM((model_width, hidden_n), bf16),
            pltpu.VMEM((hidden_n, model_width), bf16),
            pltpu.VMEM((n_tp - 1, seq_count, chan), bf16),
            pltpu.VMEM((n_tp - 1, seq_count, local_width), bf16),
            pltpu.VMEM((n_tp - 1, seq_count, local_width), bf16),
            pltpu.VMEM((experts,) + block, bf16),
            pltpu.VMEM((n_tp, experts) + block, bf16),
            pltpu.VMEM((slots, model_width), bf16),
            pltpu.VMEM((n_tp - 1, experts) + block, bf16),
            pltpu.VMEM((experts,) + block, bf16),
            pltpu.VMEM((experts, n_tp - 1) + block, bf16),
            pltpu.VMEM((experts,) + block, bf16),
            pltpu.VMEM((experts,) + block, bf16),
            dma((3,)),
            dma((n_tp - 1,)),
            dma((n_tp - 1,)),
            dma((n_tp - 1,)),
            dma((n_tp - 1,)),
            dma,
            dma((experts - 1,)),
            dma((n_tp - 1,)),
            dma((n_tp - 1,)),
            dma((n_tp - 1,)),
            dma((experts,)),
            dma,
            dma((experts - 1,)),
        ],
        compiler_params=pltpu.CompilerParams(
            collective_id=0, has_side_effects=True, vmem_limit_bytes=40 * 1024 * 1024
        ),
    )(
        mixed_in,
        tokens,
        glu_weight,
        glu_bias[None, :],
        out_weight,
        ffn_gain[None, :],
        select.astype(bf16),
        combine,
        expert_gate,
        expert_up,
        expert_down,
    )
    return (mixed, new_re, new_im)


def solution(mesh):
    in_specs = (
        P("ep", None),
        P(),
        P(None, "tp"),
        P("tp", None),
        P("tp", None),
        P("tp"),
        P("tp", None, None),
        P("tp", None, None),
        P("tp", None, None),
        P("tp", None, None),
        P("tp", None),
        P("ep", "tp", None),
        P("ep", "tp", None),
        P(None, "tp"),
        P("tp"),
        P("tp", None),
        P(),
        P("ep", None),
        P("ep", None),
        P("ep", None, "tp"),
        P("ep", None, "tp"),
        P("ep", "tp", None),
    )
    out_specs = (P("ep", "tp"), P("ep", "tp", None), P("ep", "tp", None))
    return jax.shard_map(local, mesh=mesh, in_specs=in_specs, out_specs=out_specs, check_vma=False)
```

```python
import functools
import jax
import jax.numpy as jnp
from jax import lax
from jax.experimental import pallas as pl
from jax.experimental.pallas import tpu as pltpu
from jax.sharding import PartitionSpec as P

norm_eps = 1e-06
MESH = pl.DeviceIdType.MESH


def rms_scale(rows, gain):
    values = rows.astype(jnp.float32)
    scaled = values * lax.rsqrt(jnp.mean(values * values, axis=-1, keepdims=True) + norm_eps)
    return (scaled * gain).astype(jnp.bfloat16)


def remote(src, dst, send, recv, axis, peer):
    copy = pltpu.make_async_remote_copy(
        src_ref=src,
        dst_ref=dst,
        send_sem=send,
        recv_sem=recv,
        device_id={axis: peer},
        device_id_type=MESH,
    )
    copy.start()


def drain(ref, sem):
    pltpu.make_async_copy(ref, ref, sem).wait()


def near_first(index, count):
    half = (index + 1) // 2
    odd = index % 2
    return half * odd + (count - half) * (1 - odd)


def exchange(
    n_tp,
    n_ep,
    tokens_ref,
    mix_gain_ref,
    w_in_ref,
    decay_ref,
    freq_ref,
    log_step_ref,
    in_re_ref,
    in_im_ref,
    out_re_ref,
    out_im_ref,
    skip_ref,
    bias_ref,
    gain_ref,
    route_ref,
    weight_ref,
    state_re_hbm,
    state_im_hbm,
    glu_hbm,
    out_w_hbm,
    gate_hbm,
    up_hbm,
    down_hbm,
    out_ref,
    new_re_hbm,
    new_im_hbm,
    state_re,
    state_im,
    mixed_ref,
    glu_ref,
    out_w_ref,
    gate_w,
    up_w,
    down_w,
    ag_buf,
    rs_out,
    rs_in,
    disp,
    rows,
    xn,
    back_out,
    back_own,
    back_in,
    ret_out,
    ret_in,
    w_sem,
    state_sem,
    new_sem,
    ag_s,
    ag_r,
    rs_s,
    rs_r,
    disp_s,
    disp_r,
    fwd_s,
    fwd_r,
    back_s,
    back_r,
    ret_s,
    ret_r,
):
    tp = lax.axis_index("tp")
    ep = lax.axis_index("ep")
    seqs, chan = mixed_ref.shape
    width = out_ref.shape[1]
    blocks = rows.shape[2]
    slot_rows = blocks * 8
    slots = n_ep * slot_rows
    hidden_n = gate_w.shape[1]
    f32 = jnp.float32
    bf16 = jnp.bfloat16
    groups, places, entries = in_re_ref.shape

    @pl.loop(0, groups)
    def _(g):
        for i, (far, near) in enumerate(((state_re_hbm, state_re), (state_im_hbm, state_im))):
            pltpu.make_async_copy(far.at[:, g, :], near.at[g], state_sem.at[i]).start()

    loads = [
        pltpu.make_async_copy(src, dst, w_sem.at[i])
        for i, (src, dst) in enumerate(
            (
                (glu_hbm, glu_ref),
                (out_w_hbm, out_w_ref),
                (gate_hbm.at[0], gate_w),
                (up_hbm.at[0], up_w),
                (down_hbm.at[0], down_w),
            )
        )
    ]
    for load in loads:
        load.start()

    barrier = pltpu.get_barrier_semaphore()

    @pl.loop(1, n_tp)
    def _(k):
        pl.semaphore_signal(
            barrier, inc=1, device_id={"tp": lax.rem(tp + k, n_tp)}, device_id_type=MESH
        )

    @pl.loop(1, n_ep)
    def _(k):
        pl.semaphore_signal(
            barrier, inc=1, device_id={"ep": lax.rem(ep + k, n_ep)}, device_id_type=MESH
        )

    diagonal = lax.broadcasted_iota(jnp.int32, (groups, groups), 0)
    diagonal = diagonal == lax.broadcasted_iota(jnp.int32, (groups, groups), 1)
    log_step = jnp.sum(jnp.where(diagonal, log_step_ref[...], 0.0), axis=1, keepdims=True)
    step = jnp.exp(log_step)
    decay = decay_ref[...]
    freq = freq_ref[...]
    magnitude = jnp.exp(decay * step)
    turn_re = magnitude * jnp.cos(freq * step)
    turn_im = magnitude * jnp.sin(freq * step)
    denom = decay * decay + freq * freq
    coef_re = ((turn_re - 1.0) * decay + turn_im * freq) / denom
    coef_im = (turn_im * decay - (turn_re - 1.0) * freq) / denom

    def lane_group(shape):
        lane = lax.broadcasted_iota(jnp.int32, shape, len(shape) - 1)
        first = lax.broadcasted_iota(jnp.int32, shape, 0) * places
        return (lane >= first) & (lane < first + places)

    spread = lax.broadcasted_iota(jnp.int32, (places, chan), 1) % places
    spread = spread == lax.broadcasted_iota(jnp.int32, (places, chan), 0)
    skip = jnp.dot(
        skip_ref[...],
        spread.astype(f32),
        precision=lax.Precision.HIGHEST,
        preferred_element_type=f32,
    )
    skip = jnp.sum(jnp.where(lane_group((groups, chan)), skip, 0.0), axis=0, keepdims=True)

    normed = rms_scale(tokens_ref[...], mix_gain_ref[...])
    drive = jnp.dot(normed, w_in_ref[...], preferred_element_type=f32).astype(bf16)
    own_group = lane_group((groups, seqs, chan))
    apart = jnp.where(own_group, drive.astype(f32)[None], 0.0).astype(bf16)
    apart = apart.reshape(groups * seqs, chan)

    def driven(ref):
        weight = ref[...].astype(f32).reshape(chan, entries).astype(bf16)
        value = jnp.dot(apart, weight, preferred_element_type=f32)
        return value.reshape(groups, seqs, entries)

    drive_re, drive_im = driven(in_re_ref), driven(in_im_ref)
    turn_re, turn_im = turn_re[:, None, :], turn_im[:, None, :]
    coef_re, coef_im = coef_re[:, None, :], coef_im[:, None, :]
    drain(state_re, state_sem.at[0])
    drain(state_im, state_sem.at[1])
    old_re, old_im = state_re[...], state_im[...]
    new_re = turn_re * old_re - turn_im * old_im + (coef_re * drive_re - coef_im * drive_im)
    new_im = turn_re * old_im + turn_im * old_re + (coef_re * drive_im + coef_im * drive_re)
    state_re[...] = new_re
    state_im[...] = new_im

    def read_out(value, ref):
        weight = ref[...].astype(f32).reshape(chan, entries).astype(bf16)
        value = value.reshape(groups * seqs, entries)
        high = value.astype(bf16)
        low = (value - high.astype(f32)).astype(bf16)
        dims = (((1,), (1,)), ((), ()))
        total = lax.dot_general(high, weight, dims, preferred_element_type=f32)
        return total + lax.dot_general(low, weight, dims, preferred_element_type=f32)

    read = read_out(new_re, out_re_ref) - read_out(new_im, out_im_ref)
    read = jnp.where(own_group, read.reshape(groups, seqs, chan), 0.0)
    read = jnp.sum(read, axis=0) + skip * drive.astype(f32)
    mixed = jax.nn.gelu(read).astype(bf16)
    mixed_ref[...] = mixed

    pl.semaphore_wait(barrier, n_tp + n_ep - 2)

    def peer_at(k):
        return lax.rem(tp + k, n_tp)

    def source_at(k):
        return lax.rem(tp + n_tp - k, n_tp)

    for k in range(1, n_tp):
        remote(mixed_ref, ag_buf.at[k - 1], ag_s.at[k - 1], ag_r.at[k - 1], "tp", peer_at(k))

    @pl.loop(0, groups)
    def _(g):
        for i, (near, far) in enumerate(((state_re, new_re_hbm), (state_im, new_im_hbm))):
            pltpu.make_async_copy(near.at[g], far.at[:, g, :], new_sem.at[i]).start()

    def one_hot(index, size):
        return lax.broadcasted_iota(jnp.int32, (seqs, size), 1).astype(f32) == index

    choices = [route_ref[:, k : k + 1].astype(f32) for k in range(route_ref.shape[1])]
    hits = [one_hot(choice, n_ep).astype(f32) for choice in choices]
    earlier = lax.broadcasted_iota(jnp.int32, (seqs, seqs), 1)
    earlier = earlier < lax.broadcasted_iota(jnp.int32, (seqs, seqs), 0)
    before = jnp.dot(
        earlier.astype(f32).astype(bf16), sum(hits).astype(bf16), preferred_element_type=f32
    )
    select = jnp.zeros((seqs, slots), f32)
    combine = jnp.zeros((seqs, slots), f32)
    for k, choice in enumerate(choices):
        rank = jnp.sum(before * hits[k], axis=1, keepdims=True)
        pick = one_hot(choice * slot_rows + rank, slots)
        select = jnp.where(pick, 1.0, select)
        combine = jnp.where(pick, weight_ref[:, k : k + 1], combine)

    def glu_rows(owner):
        return glu_ref[pl.ds(pl.multiple_of(owner * chan, chan), chan), :]

    loads[0].wait()
    gate = jnp.dot(mixed, glu_rows(tp), preferred_element_type=f32) + bias_ref[...]
    for k in range(1, n_tp):
        drain(ag_buf.at[k - 1], ag_r.at[k - 1])
        gate += jnp.dot(ag_buf[k - 1], glu_rows(source_at(k)), preferred_element_type=f32)
    gated = (mixed.astype(f32) * jax.nn.sigmoid(gate)).astype(bf16)

    loads[1].wait()

    def columns(owner):
        return pl.ds(pl.multiple_of(owner * width, width), width)

    for k in range(1, n_tp):
        part = jnp.dot(gated, out_w_ref[:, columns(peer_at(k))], preferred_element_type=f32)
        rs_out[k - 1] = part.astype(bf16)
        remote(
            rs_out.at[k - 1], rs_in.at[k - 1], rs_s.at[k - 1], rs_r.at[k - 1], "tp", peer_at(k)
        )
    total = jnp.dot(gated, out_w_ref[:, columns(tp)], preferred_element_type=f32)
    total = total.astype(bf16).astype(f32)
    for k in range(1, n_tp):
        drain(rs_in.at[k - 1], rs_r.at[k - 1])
        total += rs_in[k - 1].astype(f32)
    resid = (tokens_ref[:, columns(tp)].astype(f32) + total).astype(bf16)

    picked = lax.dot_general(
        select.astype(bf16), resid, (((0,), (0,)), ((), ())), preferred_element_type=f32
    )
    disp[...] = picked.reshape(n_ep, blocks, 8, width).astype(bf16)

    @pl.loop(1, n_ep)
    def _(i):
        to = lax.rem(ep + near_first(i, n_ep), n_ep)
        remote(disp.at[to], rows.at[tp, ep], disp_s, disp_r.at[i - 1], "ep", to)

    rows[tp, ep] = disp[ep]

    def forward(block):
        for k in range(1, n_tp):
            here = rows.at[tp, block]
            remote(here, here, fwd_s.at[k - 1], fwd_r.at[k - 1], "tp", peer_at(k))

    for k in range(1, n_tp):
        remote(
            disp.at[ep], rows.at[tp, ep], fwd_s.at[k - 1], fwd_r.at[k - 1], "tp", peer_at(k)
        )

    @pl.loop(1, n_ep)
    def _(i):
        block = lax.rem(ep + n_ep - near_first(i, n_ep), n_ep)
        drain(rows.at[tp, block], disp_r.at[i - 1])
        forward(block)

    def row_values(owner):
        return rows[owner].astype(f32).reshape(slots, width)

    values = row_values(tp)
    squares = jnp.sum(values * values, axis=1, keepdims=True)
    for k in range(1, n_tp):
        drain(rows.at[source_at(k)], fwd_r.at[k - 1])
        values = row_values(source_at(k))
        squares += jnp.sum(values * values, axis=1, keepdims=True)
    scale = lax.rsqrt(squares / (n_tp * width) + norm_eps)
    for owner in range(n_tp):
        cols = pl.ds(owner * width, width)
        xn[:, cols] = (row_values(owner) * scale * gain_ref[:, cols]).astype(bf16)

    loads[2].wait()
    loads[3].wait()
    pieces = []
    for start in range(0, hidden_n, 256):
        cols = pl.ds(start, min(256, hidden_n - start))
        gate_h = jnp.dot(xn[...], gate_w[:, cols], preferred_element_type=f32)
        up_h = jnp.dot(xn[...], up_w[:, cols], preferred_element_type=f32)
        pieces.append((jax.nn.silu(gate_h) * up_h).astype(bf16))
    hidden = jnp.concatenate(pieces, axis=1)
    loads[4].wait()

    def down(owner):
        part = jnp.dot(hidden, down_w[:, columns(owner)], preferred_element_type=f32)
        return part.reshape(n_ep, blocks, 8, width).astype(bf16)

    for k in range(1, n_tp):
        back_out[k - 1] = down(peer_at(k))

        @pl.loop(1, n_ep + 1)
        def _(i):
            block = lax.rem(ep + near_first(i, n_ep) * (i // n_ep * -1 + 1), n_ep)
            remote(
                back_out.at[k - 1, block],
                back_in.at[block, k - 1],
                back_s.at[k - 1],
                back_r.at[block],
                "tp",
                peer_at(k),
            )

    back_own[...] = down(tp)

    def settled(block):
        drain(back_in.at[block], back_r.at[block])
        result = back_own[block].astype(f32)
        for k in range(1, n_tp):
            result += back_in[block, k - 1].astype(f32)
        return result.astype(bf16)

    @pl.loop(1, n_ep)
    def _(i):
        to = lax.rem(ep + near_first(i, n_ep), n_ep)
        ret_out[to] = settled(to)
        remote(ret_out.at[to], ret_in.at[ep], ret_s, ret_r.at[i - 1], "ep", to)

    ret_in[ep] = settled(ep)

    @pl.loop(1, n_ep)
    def _(i):
        block = lax.rem(ep + n_ep - near_first(i, n_ep), n_ep)
        drain(ret_in.at[block], ret_r.at[i - 1])

    returned = ret_in[...].astype(f32).reshape(slots, width).astype(bf16)
    high = combine.astype(bf16)
    low = (combine - high.astype(f32)).astype(bf16)
    expert_total = jnp.dot(high, returned, preferred_element_type=f32)
    expert_total += jnp.dot(low, returned, preferred_element_type=f32)
    out_ref[...] = (resid.astype(f32) + expert_total).astype(bf16)

    for k in range(1, n_tp):
        drain(mixed_ref, ag_s.at[k - 1])
        drain(rs_out.at[k - 1], rs_s.at[k - 1])
        drain(rows.at[0], fwd_s.at[k - 1])
        drain(back_out.at[k - 1], back_s.at[k - 1])
    drain(disp.at[pl.ds(0, n_ep - 1)], disp_s)
    drain(ret_out.at[pl.ds(0, n_ep - 1)], ret_s)
    drain(state_re, new_sem.at[0])
    drain(state_im, new_sem.at[1])


def local(
    tokens,
    mix_gain,
    w_in,
    decay_re,
    freq,
    log_step,
    in_re,
    in_im,
    out_re,
    out_im,
    skip,
    state_re,
    state_im,
    glu_weight,
    glu_bias,
    out_weight,
    ffn_gain,
    route,
    route_weight,
    expert_gate,
    expert_up,
    expert_down,
):
    seq_count, model_width = tokens.shape
    groups_local = decay_re.shape[0]
    n_tp = lax.axis_size("tp")
    experts = lax.axis_size("ep")
    local_width = model_width // n_tp
    top_count = route.shape[1]
    hidden_n = expert_gate.shape[2]
    slot_cap = (3 * seq_count * top_count + 2 * experts - 1) // (2 * experts)
    slot_rows = (slot_cap + 7) // 8 * 8
    slots = experts * slot_rows
    chan = w_in.shape[1]
    state_block = (groups_local, seq_count, state_re.shape[2])
    block = (slot_rows // 8, 8, local_width)
    bf16 = jnp.bfloat16
    dma = pltpu.SemaphoreType.DMA
    vmem = pl.BlockSpec(memory_space=pltpu.VMEM)
    anyplace = pl.BlockSpec(memory_space=pl.ANY)
    return pl.pallas_call(
        functools.partial(exchange, n_tp, experts),
        out_shape=(
            jax.ShapeDtypeStruct((seq_count, local_width), bf16),
            jax.ShapeDtypeStruct(state_re.shape, jnp.float32),
            jax.ShapeDtypeStruct(state_im.shape, jnp.float32),
        ),
        in_specs=[vmem] * 15 + [anyplace] * 7,
        out_specs=(vmem, anyplace, anyplace),
        scratch_shapes=[
            pltpu.VMEM(state_block, jnp.float32),
            pltpu.VMEM(state_block, jnp.float32),
            pltpu.VMEM((seq_count, chan), bf16),
            pltpu.VMEM(glu_weight.shape, bf16),
            pltpu.VMEM(out_weight.shape, bf16),
            pltpu.VMEM((model_width, hidden_n), bf16),
            pltpu.VMEM((model_width, hidden_n), bf16),
            pltpu.VMEM((hidden_n, model_width), bf16),
            pltpu.VMEM((n_tp - 1, seq_count, chan), bf16),
            pltpu.VMEM((n_tp - 1, seq_count, local_width), bf16),
            pltpu.VMEM((n_tp - 1, seq_count, local_width), bf16),
            pltpu.VMEM((experts,) + block, bf16),
            pltpu.VMEM((n_tp, experts) + block, bf16),
            pltpu.VMEM((slots, model_width), bf16),
            pltpu.VMEM((n_tp - 1, experts) + block, bf16),
            pltpu.VMEM((experts,) + block, bf16),
            pltpu.VMEM((experts, n_tp - 1) + block, bf16),
            pltpu.VMEM((experts,) + block, bf16),
            pltpu.VMEM((experts,) + block, bf16),
            dma((5,)),
            dma((2,)),
            dma((2,)),
            dma((n_tp - 1,)),
            dma((n_tp - 1,)),
            dma((n_tp - 1,)),
            dma((n_tp - 1,)),
            dma,
            dma((experts - 1,)),
            dma((n_tp - 1,)),
            dma((n_tp - 1,)),
            dma((n_tp - 1,)),
            dma((experts,)),
            dma,
            dma((experts - 1,)),
        ],
        compiler_params=pltpu.CompilerParams(
            collective_id=0, has_side_effects=True, vmem_limit_bytes=61 * 1024 * 1024
        ),
    )(
        tokens,
        mix_gain[None, :],
        w_in,
        decay_re,
        freq,
        log_step[None, :],
        in_re,
        in_im,
        out_re,
        out_im,
        skip,
        glu_bias[None, :],
        ffn_gain[None, :],
        route,
        route_weight,
        state_re,
        state_im,
        glu_weight,
        out_weight,
        expert_gate,
        expert_up,
        expert_down,
    )


def solution(mesh):
    in_specs = (
        P("ep", None),
        P(),
        P(None, "tp"),
        P("tp", None),
        P("tp", None),
        P("tp"),
        P("tp", None, None),
        P("tp", None, None),
        P("tp", None, None),
        P("tp", None, None),
        P("tp", None),
        P("ep", "tp", None),
        P("ep", "tp", None),
        P(None, "tp"),
        P("tp"),
        P("tp", None),
        P(),
        P("ep", None),
        P("ep", None),
        P("ep", None, "tp"),
        P("ep", None, "tp"),
        P("ep", "tp", None),
    )
    out_specs = (P("ep", "tp"), P("ep", "tp", None), P("ep", "tp", None))
    return jax.shard_map(local, mesh=mesh, in_specs=in_specs, out_specs=out_specs, check_vma=False)
```

```python
import functools
import jax
import jax.numpy as jnp
from jax import lax
from jax.experimental import pallas as pl
from jax.experimental.pallas import tpu as pltpu
from jax.sharding import PartitionSpec as P

norm_eps = 1e-06
MESH = pl.DeviceIdType.MESH


def rms_scale(rows, gain):
    values = rows.astype(jnp.float32)
    scaled = values * lax.rsqrt(jnp.mean(values * values, axis=-1, keepdims=True) + norm_eps)
    return (scaled * gain).astype(jnp.bfloat16)


def state_kernel(
    tokens_ref,
    mix_gain_ref,
    w_in_ref,
    decay_ref,
    freq_ref,
    log_step_ref,
    in_re_ref,
    in_im_ref,
    out_re_ref,
    out_im_ref,
    skip_ref,
    state_re_hbm,
    state_im_hbm,
    mixed_ref,
    new_re_hbm,
    new_im_hbm,
    state_re,
    state_im,
    state_sem,
    new_sem,
):
    f32 = jnp.float32
    bf16 = jnp.bfloat16
    groups, places, entries = in_re_ref.shape
    seqs, chan = mixed_ref.shape

    @pl.loop(0, groups)
    def _(g):
        for i, (far, near) in enumerate(((state_re_hbm, state_re), (state_im_hbm, state_im))):
            pltpu.make_async_copy(far.at[:, g, :], near.at[g], state_sem.at[i]).start()

    diagonal = lax.broadcasted_iota(jnp.int32, (groups, groups), 0)
    diagonal = diagonal == lax.broadcasted_iota(jnp.int32, (groups, groups), 1)
    log_step = jnp.sum(jnp.where(diagonal, log_step_ref[...], 0.0), axis=1, keepdims=True)
    step = jnp.exp(log_step)
    decay = decay_ref[...]
    freq = freq_ref[...]
    magnitude = jnp.exp(decay * step)
    turn_re = magnitude * jnp.cos(freq * step)
    turn_im = magnitude * jnp.sin(freq * step)
    denom = decay * decay + freq * freq
    coef_re = ((turn_re - 1.0) * decay + turn_im * freq) / denom
    coef_im = (turn_im * decay - (turn_re - 1.0) * freq) / denom

    def lane_group(shape):
        lane = lax.broadcasted_iota(jnp.int32, shape, len(shape) - 1)
        first = lax.broadcasted_iota(jnp.int32, shape, 0) * places
        return (lane >= first) & (lane < first + places)

    spread = lax.broadcasted_iota(jnp.int32, (places, chan), 1) % places
    spread = spread == lax.broadcasted_iota(jnp.int32, (places, chan), 0)
    skip = jnp.dot(
        skip_ref[...],
        spread.astype(f32),
        precision=lax.Precision.HIGHEST,
        preferred_element_type=f32,
    )
    skip = jnp.sum(jnp.where(lane_group((groups, chan)), skip, 0.0), axis=0, keepdims=True)

    normed = rms_scale(tokens_ref[...], mix_gain_ref[...])
    drive = jnp.dot(normed, w_in_ref[...], preferred_element_type=f32).astype(bf16)
    own_group = lane_group((groups, seqs, chan))
    apart = jnp.where(own_group, drive.astype(f32)[None], 0.0).astype(bf16)
    apart = apart.reshape(groups * seqs, chan)

    def driven(ref):
        weight = ref[...].astype(f32).reshape(chan, entries).astype(bf16)
        value = jnp.dot(apart, weight, preferred_element_type=f32)
        return value.reshape(groups, seqs, entries)

    drive_re, drive_im = driven(in_re_ref), driven(in_im_ref)
    turn_re, turn_im = turn_re[:, None, :], turn_im[:, None, :]
    coef_re, coef_im = coef_re[:, None, :], coef_im[:, None, :]
    drain(state_re, state_sem.at[0])
    drain(state_im, state_sem.at[1])
    old_re, old_im = state_re[...], state_im[...]
    new_re = turn_re * old_re - turn_im * old_im + (coef_re * drive_re - coef_im * drive_im)
    new_im = turn_re * old_im + turn_im * old_re + (coef_re * drive_im + coef_im * drive_re)
    state_re[...] = new_re
    state_im[...] = new_im

    @pl.loop(0, groups)
    def _(g):
        for i, (near, far) in enumerate(((state_re, new_re_hbm), (state_im, new_im_hbm))):
            pltpu.make_async_copy(near.at[g], far.at[:, g, :], new_sem.at[i]).start()

    def read_out(value, ref):
        weight = ref[...].astype(f32).reshape(chan, entries).astype(bf16)
        value = value.reshape(groups * seqs, entries)
        high = value.astype(bf16)
        low = (value - high.astype(f32)).astype(bf16)
        dims = (((1,), (1,)), ((), ()))
        total = lax.dot_general(high, weight, dims, preferred_element_type=f32)
        return total + lax.dot_general(low, weight, dims, preferred_element_type=f32)

    read = read_out(new_re, out_re_ref) - read_out(new_im, out_im_ref)
    read = jnp.where(own_group, read.reshape(groups, seqs, chan), 0.0)
    read = jnp.sum(read, axis=0) + skip * drive.astype(f32)
    mixed = jax.nn.gelu(read).astype(bf16)
    mixed_ref[...] = mixed
    drain(state_re, new_sem.at[0])
    drain(state_im, new_sem.at[1])


def remote(src, dst, send, recv, axis, peer):
    copy = pltpu.make_async_remote_copy(
        src_ref=src,
        dst_ref=dst,
        send_sem=send,
        recv_sem=recv,
        device_id={axis: peer},
        device_id_type=MESH,
    )
    copy.start()


def drain(ref, sem):
    pltpu.make_async_copy(ref, ref, sem).wait()


def near_first(index, count):
    half = (index + 1) // 2
    odd = index % 2
    return half * odd + (count - half) * (1 - odd)


def exchange(
    n_tp,
    n_ep,
    mixed_ref,
    tokens_ref,
    bias_ref,
    gain_ref,
    route_ref,
    weight_ref,
    glu_hbm,
    out_w_hbm,
    gate_hbm,
    up_hbm,
    down_hbm,
    out_ref,
    glu_ref,
    out_w_ref,
    gate_w,
    up_w,
    down_w,
    ag_buf,
    rs_out,
    rs_in,
    disp,
    rows,
    xn,
    back_out,
    back_own,
    back_in,
    ret_out,
    ret_in,
    w_sem,
    ag_s,
    ag_r,
    rs_s,
    rs_r,
    disp_s,
    disp_r,
    fwd_s,
    fwd_r,
    back_s,
    back_r,
    ret_s,
    ret_r,
):
    tp = lax.axis_index("tp")
    ep = lax.axis_index("ep")
    seqs, chan = mixed_ref.shape
    width = out_ref.shape[1]
    blocks = rows.shape[2]
    slot_rows = blocks * 8
    slots = n_ep * slot_rows
    hidden_n = gate_w.shape[1]
    f32 = jnp.float32
    bf16 = jnp.bfloat16

    loads = [
        pltpu.make_async_copy(src, dst, w_sem.at[i])
        for i, (src, dst) in enumerate(
            (
                (glu_hbm, glu_ref),
                (out_w_hbm, out_w_ref),
                (gate_hbm.at[0], gate_w),
                (up_hbm.at[0], up_w),
                (down_hbm.at[0], down_w),
            )
        )
    ]
    for load in loads:
        load.start()

    barrier = pltpu.get_barrier_semaphore()

    @pl.loop(1, n_tp)
    def _(k):
        pl.semaphore_signal(
            barrier, inc=1, device_id={"tp": lax.rem(tp + k, n_tp)}, device_id_type=MESH
        )

    @pl.loop(1, n_ep)
    def _(k):
        pl.semaphore_signal(
            barrier, inc=1, device_id={"ep": lax.rem(ep + k, n_ep)}, device_id_type=MESH
        )

    pl.semaphore_wait(barrier, n_tp + n_ep - 2)

    def peer_at(k):
        return lax.rem(tp + k, n_tp)

    def source_at(k):
        return lax.rem(tp + n_tp - k, n_tp)

    for k in range(1, n_tp):
        remote(mixed_ref, ag_buf.at[k - 1], ag_s.at[k - 1], ag_r.at[k - 1], "tp", peer_at(k))

    def one_hot(index, size):
        return lax.broadcasted_iota(jnp.int32, (seqs, size), 1).astype(f32) == index

    row = lax.broadcasted_iota(jnp.int32, (seqs, seqs), 0)
    lane = lax.broadcasted_iota(jnp.int32, (seqs, seqs), 1)

    def upright(ref, k):
        value = ref[k : k + 1, :].astype(f32)
        return jnp.sum(jnp.where(row == lane, value, 0.0), axis=1, keepdims=True)

    choices = [upright(route_ref, k) for k in range(route_ref.shape[0])]
    hits = [one_hot(choice, n_ep).astype(f32) for choice in choices]
    earlier = jnp.where(lane < row, 1.0, 0.0).astype(bf16)
    before = jnp.dot(earlier, sum(hits).astype(bf16), preferred_element_type=f32)
    select = jnp.zeros((seqs, slots), f32)
    combine = jnp.zeros((seqs, slots), f32)
    for k, choice in enumerate(choices):
        rank = jnp.sum(before * hits[k], axis=1, keepdims=True)
        pick = one_hot(choice * slot_rows + rank, slots)
        select = jnp.where(pick, 1.0, select)
        combine = jnp.where(pick, upright(weight_ref, k), combine)

    mixed = mixed_ref[...]

    def glu_rows(owner):
        return glu_ref[pl.ds(pl.multiple_of(owner * chan, chan), chan), :]

    loads[0].wait()
    gate = jnp.dot(mixed, glu_rows(tp), preferred_element_type=f32) + bias_ref[...]
    for k in range(1, n_tp):
        drain(ag_buf.at[k - 1], ag_r.at[k - 1])
        gate += jnp.dot(ag_buf[k - 1], glu_rows(source_at(k)), preferred_element_type=f32)
    gated = (mixed.astype(f32) * jax.nn.sigmoid(gate)).astype(bf16)

    loads[1].wait()

    def columns(owner):
        return pl.ds(pl.multiple_of(owner * width, width), width)

    for k in range(1, n_tp):
        part = jnp.dot(gated, out_w_ref[:, columns(peer_at(k))], preferred_element_type=f32)
        rs_out[k - 1] = part.astype(bf16)
        remote(
            rs_out.at[k - 1], rs_in.at[k - 1], rs_s.at[k - 1], rs_r.at[k - 1], "tp", peer_at(k)
        )
    total = jnp.dot(gated, out_w_ref[:, columns(tp)], preferred_element_type=f32)
    total = total.astype(bf16).astype(f32)
    for k in range(1, n_tp):
        drain(rs_in.at[k - 1], rs_r.at[k - 1])
        total += rs_in[k - 1].astype(f32)
    resid = (tokens_ref[:, columns(tp)].astype(f32) + total).astype(bf16)

    picked = lax.dot_general(
        select.astype(bf16), resid, (((0,), (0,)), ((), ())), preferred_element_type=f32
    )
    disp[...] = picked.reshape(n_ep, blocks, 8, width).astype(bf16)

    @pl.loop(1, n_ep)
    def _(i):
        to = lax.rem(ep + near_first(i, n_ep), n_ep)
        remote(disp.at[to], rows.at[tp, i], disp_s, disp_r.at[i - 1], "ep", to)

    half = n_ep // 2
    for k in range(1, n_tp):
        remote(disp.at[ep], rows.at[tp, 0], fwd_s.at[k - 1], fwd_r.at[0, k - 1], "tp", peer_at(k))
    rows[tp, 0] = disp[ep]

    @pl.loop(1, n_ep)
    def _(i):
        here = rows.at[tp, i]
        drain(here, disp_r.at[i - 1])
        for k in range(1, n_tp):
            remote(here, here, fwd_s.at[k - 1], fwd_r.at[i // half, k - 1], "tp", peer_at(k))

    for part in range(2):
        span = pl.ds(part * half, half)

        def row_values(owner):
            return rows[owner, span].astype(f32).reshape(slots // 2, width)

        values = row_values(tp)
        squares = jnp.sum(values * values, axis=1, keepdims=True)
        for k in range(1, n_tp):
            drain(rows.at[source_at(k), span], fwd_r.at[part, k - 1])
            values = row_values(source_at(k))
            squares += jnp.sum(values * values, axis=1, keepdims=True)
        scale = lax.rsqrt(squares / (n_tp * width) + norm_eps)
        for owner in range(n_tp):
            cols = pl.ds(owner * width, width)
            xn[:, cols] = (row_values(owner) * scale * gain_ref[:, cols]).astype(bf16)

        if part == 0:
            loads[2].wait()
            loads[3].wait()
        pieces = []
        for start in range(0, hidden_n, 256):
            cols = pl.ds(start, min(256, hidden_n - start))
            gate_h = jnp.dot(xn[...], gate_w[:, cols], preferred_element_type=f32)
            up_h = jnp.dot(xn[...], up_w[:, cols], preferred_element_type=f32)
            pieces.append((jax.nn.silu(gate_h) * up_h).astype(bf16))
        hidden = jnp.concatenate(pieces, axis=1)
        if part == 0:
            loads[4].wait()

        def down(owner):
            value = jnp.dot(hidden, down_w[:, columns(owner)], preferred_element_type=f32)
            return value.reshape(half, blocks, 8, width).astype(bf16)

        for k in range(1, n_tp):
            back_out[k - 1, span] = down(peer_at(k))

            @pl.loop(part * half, part * half + half)
            def _(i):
                remote(
                    back_out.at[k - 1, i],
                    back_in.at[i, k - 1],
                    back_s.at[k - 1],
                    back_r.at[i],
                    "tp",
                    peer_at(k),
                )

        back_own[span] = down(tp)

    def settled(i):
        drain(back_in.at[i], back_r.at[i])
        result = back_own[i].astype(f32)
        for k in range(1, n_tp):
            result += back_in[i, k - 1].astype(f32)
        return result.astype(bf16)

    @pl.loop(1, n_ep)
    def _(i):
        to = lax.rem(ep + n_ep - near_first(i, n_ep), n_ep)
        ret_out[to] = settled(i)
        remote(ret_out.at[to], ret_in.at[ep], ret_s, ret_r.at[i - 1], "ep", to)

    ret_in[ep] = settled(0)

    @pl.loop(1, n_ep)
    def _(i):
        block = lax.rem(ep + near_first(i, n_ep), n_ep)
        drain(ret_in.at[block], ret_r.at[i - 1])

    returned = ret_in[...].astype(f32).reshape(slots, width).astype(bf16)
    high = combine.astype(bf16)
    low = (combine - high.astype(f32)).astype(bf16)
    expert_total = jnp.dot(high, returned, preferred_element_type=f32)
    expert_total += jnp.dot(low, returned, preferred_element_type=f32)
    out_ref[...] = (resid.astype(f32) + expert_total).astype(bf16)

    for k in range(1, n_tp):
        drain(mixed_ref, ag_s.at[k - 1])
        drain(rs_out.at[k - 1], rs_s.at[k - 1])
        drain(rows.at[0], fwd_s.at[k - 1])
        drain(back_out.at[k - 1], back_s.at[k - 1])
    drain(disp.at[pl.ds(0, n_ep - 1)], disp_s)
    drain(ret_out.at[pl.ds(0, n_ep - 1)], ret_s)


def local(
    tokens,
    mix_gain,
    w_in,
    decay_re,
    freq,
    log_step,
    in_re,
    in_im,
    out_re,
    out_im,
    skip,
    state_re,
    state_im,
    glu_weight,
    glu_bias,
    out_weight,
    ffn_gain,
    route,
    route_weight,
    expert_gate,
    expert_up,
    expert_down,
):
    seq_count, model_width = tokens.shape
    groups_local = decay_re.shape[0]
    n_tp = lax.axis_size("tp")
    experts = lax.axis_size("ep")
    local_width = model_width // n_tp
    top_count = route.shape[1]
    hidden_n = expert_gate.shape[2]
    slot_cap = (3 * seq_count * top_count + 2 * experts - 1) // (2 * experts)
    slot_rows = (slot_cap + 7) // 8 * 8
    slots = experts * slot_rows
    chan = w_in.shape[1]
    state_block = (groups_local, seq_count, state_re.shape[2])
    block = (slot_rows // 8, 8, local_width)
    bf16 = jnp.bfloat16
    dma = pltpu.SemaphoreType.DMA
    vmem = pl.BlockSpec(memory_space=pltpu.VMEM)
    anyplace = pl.BlockSpec(memory_space=pl.ANY)
    mixed_in, new_re, new_im = pl.pallas_call(
        state_kernel,
        out_shape=(
            jax.ShapeDtypeStruct((seq_count, chan), bf16),
            jax.ShapeDtypeStruct(state_re.shape, jnp.float32),
            jax.ShapeDtypeStruct(state_im.shape, jnp.float32),
        ),
        in_specs=[vmem] * 11 + [anyplace] * 2,
        out_specs=(vmem, anyplace, anyplace),
        scratch_shapes=[
            pltpu.VMEM(state_block, jnp.float32),
            pltpu.VMEM(state_block, jnp.float32),
            dma((2,)),
            dma((2,)),
        ],
    )(
        tokens,
        mix_gain[None, :],
        w_in,
        decay_re,
        freq,
        log_step[None, :],
        in_re,
        in_im,
        out_re,
        out_im,
        skip,
        state_re,
        state_im,
    )
    mixed = pl.pallas_call(
        functools.partial(exchange, n_tp, experts),
        out_shape=jax.ShapeDtypeStruct((seq_count, local_width), bf16),
        in_specs=[vmem] * 6 + [anyplace] * 5,
        out_specs=vmem,
        scratch_shapes=[
            pltpu.VMEM(glu_weight.shape, bf16),
            pltpu.VMEM(out_weight.shape, bf16),
            pltpu.VMEM((model_width, hidden_n), bf16),
            pltpu.VMEM((model_width, hidden_n), bf16),
            pltpu.VMEM((hidden_n, model_width), bf16),
            pltpu.VMEM((n_tp - 1, seq_count, chan), bf16),
            pltpu.VMEM((n_tp - 1, seq_count, local_width), bf16),
            pltpu.VMEM((n_tp - 1, seq_count, local_width), bf16),
            pltpu.VMEM((experts,) + block, bf16),
            pltpu.VMEM((n_tp, experts) + block, bf16),
            pltpu.VMEM((slots // 2, model_width), bf16),
            pltpu.VMEM((n_tp - 1, experts) + block, bf16),
            pltpu.VMEM((experts,) + block, bf16),
            pltpu.VMEM((experts, n_tp - 1) + block, bf16),
            pltpu.VMEM((experts,) + block, bf16),
            pltpu.VMEM((experts,) + block, bf16),
            dma((5,)),
            dma((n_tp - 1,)),
            dma((n_tp - 1,)),
            dma((n_tp - 1,)),
            dma((n_tp - 1,)),
            dma,
            dma((experts - 1,)),
            dma((n_tp - 1,)),
            dma((2, n_tp - 1)),
            dma((n_tp - 1,)),
            dma((experts,)),
            dma,
            dma((experts - 1,)),
        ],
        compiler_params=pltpu.CompilerParams(
            collective_id=0, has_side_effects=True, vmem_limit_bytes=61 * 1024 * 1024
        ),
    )(
        mixed_in,
        tokens,
        glu_bias[None, :],
        ffn_gain[None, :],
        route.T,
        route_weight.T,
        glu_weight,
        out_weight,
        expert_gate,
        expert_up,
        expert_down,
    )
    return (mixed, new_re, new_im)


def solution(mesh):
    in_specs = (
        P("ep", None),
        P(),
        P(None, "tp"),
        P("tp", None),
        P("tp", None),
        P("tp"),
        P("tp", None, None),
        P("tp", None, None),
        P("tp", None, None),
        P("tp", None, None),
        P("tp", None),
        P("ep", "tp", None),
        P("ep", "tp", None),
        P(None, "tp"),
        P("tp"),
        P("tp", None),
        P(),
        P("ep", None),
        P("ep", None),
        P("ep", None, "tp"),
        P("ep", None, "tp"),
        P("ep", "tp", None),
    )
    out_specs = (P("ep", "tp"), P("ep", "tp", None), P("ep", "tp", None))
    return jax.shard_map(local, mesh=mesh, in_specs=in_specs, out_specs=out_specs, check_vma=False)
```
